32 devices in a mesh: sp: 4 (over z), fs: 4 (over y, x), tp: 2 (over core).
Axes of the slice: x: 2, y: 2, z: 4, core: 2. Of those that a mesh axis runs over, the one named last changes fastest.
Arguments:
- tokens: bfloat16 [4, 3072, 2048], P('fs', 'sp'), may hold values from -6 to 6
- norm_gain: float32 [2048], replicated, may hold values from 0.1 to 1.9
- w_query: bfloat16 [2048, 512], P('sp', 'tp'), may hold values from -0.125 to 0.125
- w_key: bfloat16 [2048, 512], P('sp', 'tp'), may hold values from -0.125 to 0.125
- w_value: bfloat16 [2048, 1024], P('sp', 'tp'), may hold values from -0.125 to 0.125
- w_conv_value: bfloat16 [2048, 1024], P('sp', 'tp'), may hold values from -0.125 to 0.125
- w_conv_gate: bfloat16 [2048, 1024], P('sp', 'tp'), may hold values from -0.125 to 0.125
- w_decay_low: bfloat16 [2048, 16], replicated, may hold values from -0.125 to 0.125
- w_decay_high: bfloat16 [16, 512], replicated, may hold values from -1.5 to 1.5
- gate_bias: float32 [512], replicated, may hold values from 0.5 to 10
- decay_shift: float32 [4, 3072, 512], P('fs', 'sp', 'tp'), may hold values from -0.6 to 0
- head_gain: float32 [512], replicated, may hold values from 0.1 to 1.9
- conv_taps: float32 [31, 1024], replicated, may hold values from -15 to 15
- channel_gain: float32 [1024], replicated, may hold values from 0.1 to 1.9
- w_out_attn: bfloat16 [1024, 2048], P('tp', 'sp'), may hold values from -0.125 to 0.125
- w_out_conv: bfloat16 [1024, 2048], P('tp', 'sp'), may hold values from -0.125 to 0.125
- init_state: float32 [4, 2, 256, 512], P('fs', 'tp'), may hold values from -332.55374 to 332.55374
Outputs:
- mixed: bfloat16 [4, 3072, 2048], P('fs', ('sp', 'tp'))
The draws below stay inside these ranges and needn't reach their ends.
All inputs are finite; a program needn't handle non-finite values.
Results may differ from the reference program's by a relative error of at most 0.0056.
The reference program's roundings to bfloat16 on the way (of `normed`, `low_rank`, `attn_out`, `glu` and `conv_out`) count: a program that leaves them out, or rounds other values in their place, can miss the bound.
Values may be sent and summed in bfloat16 or wider, within the bound.
No kernel may reach another device: no remote copies, remote signals or barrier semaphores. Data moves between devices by JAX's collectives and lax.ppermute only.
A program may use at most 128 MiB of HBM per device.

```python
import math
import jax
import jax.numpy as jnp
from jax import lax

D = 2048
GHEADS = 2
DK = 256
DV = 512
CW = 1024
RANK = 16
KW = 31
BLOCK = 64
T_DEV = 768
SEQS = 4
LENGTH = 3072
GKW = 512
GVW = 1024


def draw_gate_bias(key, part):
    pick_key, slow_key, fast_key = jax.random.split(jax.random.fold_in(key, 11), 3)
    share = 0.5
    chosen = jax.random.uniform(pick_key, (GKW,), jnp.float32) < share
    slow_values = jax.random.uniform(slow_key, (GKW,), jnp.float32, 8.0, 10.0)
    fast_values = jax.random.uniform(fast_key, (GKW,), jnp.float32, 0.5, 1.5)
    return jnp.where(chosen, slow_values, fast_values)


def draw_decay_shift(key, part):
    rate_key, mark_key, depth_key = jax.random.split(jax.random.fold_in(key, 23), 3)
    nblocks = LENGTH // T_DEV
    rates = jnp.exp(jax.random.uniform(rate_key, (SEQS, nblocks, 1, GKW), jnp.float32, math.log(0.2), math.log(1.0))) / LENGTH
    steady = jnp.broadcast_to(rates, (SEQS, nblocks, T_DEV, GKW)).reshape(SEQS, LENGTH, GKW)
    marks = jax.random.uniform(mark_key, (SEQS, LENGTH, 1), jnp.float32) < 3.0 / LENGTH
    depths = jax.random.uniform(depth_key, (SEQS, LENGTH, GKW), jnp.float32, 0.22, 0.5)
    return -steady - jnp.where(marks, depths, 0.0)


def draw_conv_taps(key, part):
    base_key, jitter_key = jax.random.split(jax.random.fold_in(key, 37))
    base = jnp.clip(jax.random.normal(base_key, (KW, CW), jnp.float32), -4.0, 4.0) / math.sqrt(KW)
    channel = jnp.arange(CW, dtype=jnp.float32) / CW
    jitter = jnp.exp(jax.random.uniform(jitter_key, (1, CW), jnp.float32, math.log(0.5), math.log(2.0)))
    return base * jnp.exp(math.log(10.0) * channel) * jitter


def shard_levels(rng, shape, shards, least, top_value):
    def one(dim, shards_of):
        steps = jax.random.uniform(jax.random.fold_in(jax.random.fold_in(rng, 6), dim), (shards_of,), jnp.float32, least / len(shards), top_value / len(shards))
        return jnp.repeat(jnp.exp(steps), shape[dim] // shards_of).reshape((-1,) + (1,) * (len(shape) - dim - 1))

    factor_of = one(*shards[0])
    for cut in shards[1:]:
        factor_of = factor_of * one(*cut)
    return factor_of


def noise(own_key, extent, spread, most, pieces=(), kind=jnp.bfloat16):
    drawn = spread * jax.random.normal(own_key, extent, jnp.float32)
    if pieces:
        drawn = drawn * shard_levels(own_key, extent, pieces, -0.22, 0.18)
    return jnp.clip(drawn, -most, most).astype(kind)


def setup_inputs(seed: int = 0) -> dict:
    keys = jax.random.split(jax.random.key(seed), 18)
    return {
        "tokens": noise(keys[0], (SEQS, LENGTH, D), 1.0, 6.0, ((0, 4), (1, 4))),
        "norm_gain": jnp.clip(1.0 + 0.18 * jax.random.normal(keys[1], (D,), jnp.float32), 0.1, 1.9),
        "w_query": noise(keys[2], (D, GKW), D ** -0.5, 0.125, ((0, 4), (1, 2))),
        "w_key": noise(keys[3], (D, GKW), D ** -0.5, 0.125, ((0, 4), (1, 2))),
        "w_value": noise(keys[4], (D, GVW), D ** -0.5, 0.125, ((0, 4), (1, 2))),
        "w_conv_value": noise(keys[5], (D, CW), D ** -0.5, 0.125, ((0, 4), (1, 2))),
        "w_conv_gate": noise(keys[6], (D, CW), D ** -0.5, 0.125, ((0, 4), (1, 2))),
        "w_decay_low": noise(keys[7], (D, RANK), D ** -0.5, 0.125),
        "w_decay_high": noise(keys[8], (RANK, GKW), RANK ** -0.5, 1.5),
        "gate_bias": draw_gate_bias(jax.random.fold_in(keys[17], 71), 0),
        "decay_shift": draw_decay_shift(jax.random.fold_in(keys[17], 71), 0),
        "head_gain": jnp.clip(1.0 + 0.18 * jax.random.normal(keys[11], (DV,), jnp.float32), 0.1, 1.9),
        "conv_taps": draw_conv_taps(jax.random.fold_in(keys[17], 71), 0),
        "channel_gain": jnp.clip(1.0 + 0.18 * jax.random.normal(keys[13], (CW,), jnp.float32), 0.1, 1.9),
        "w_out_attn": noise(keys[14], (GVW, D), (GVW + CW) ** -0.5, 0.125, ((0, 2), (1, 4))),
        "w_out_conv": noise(keys[15], (CW, D), (GVW + CW) ** -0.5, 0.125, ((0, 2), (1, 4))),
        "init_state": noise(keys[16], (SEQS, GHEADS, DK, DV), (LENGTH ** 0.5), 332.55374, ((0, 4), (1, 2)), jnp.float32),
    }


RMS_EPS = 1e-06
LN_EPS = 1e-05
GATE_NORMALIZER = 16.0
UPPER_PRECISION = lax.Precision.HIGHEST

def rounded(array):
    return lax.optimization_barrier(array.astype(jnp.bfloat16)).astype(jnp.float32)

def one_sequence(token_rows, shift_log, start_state, norm_gain, w_query, w_key, w_value, w_conv_value, w_conv_gate, w_decay_low, w_decay_high, gate_bias, head_gain, conv_taps, channel_gain, w_out_attn, w_out_conv):
    rows_float = token_rows.astype(jnp.float32)
    normed = (rows_float * lax.rsqrt(lax.optimization_barrier(jnp.mean(rows_float * rows_float, axis=1, keepdims=True)) + RMS_EPS) * norm_gain).astype(jnp.bfloat16)
    queries = rounded(jnp.dot(normed, w_query, preferred_element_type=jnp.float32))
    keys_proj = rounded(jnp.dot(normed, w_key, preferred_element_type=jnp.float32))
    values_proj = rounded(jnp.dot(normed, w_value, preferred_element_type=jnp.float32))
    low_rank = jnp.dot(normed, w_decay_low, preferred_element_type=jnp.float32).astype(jnp.bfloat16)
    log_decay = jax.nn.log_sigmoid(jnp.dot(low_rank, w_decay_high, preferred_element_type=jnp.float32) + gate_bias) / GATE_NORMALIZER + shift_log
    nblocks = LENGTH // BLOCK

    def blocks_of(array, width):
        return array.reshape(nblocks, BLOCK, GHEADS, width).transpose(0, 2, 1, 3)
    query_blocks = blocks_of(queries, DK) * DK ** (-0.5)
    key_blocks = blocks_of(keys_proj, DK)
    value_blocks = blocks_of(values_proj, DV)
    decay_blocks = blocks_of(log_decay, DK)
    lower = jnp.tril(jnp.ones((BLOCK, BLOCK), jnp.float32))

    def step(recurrent_state, inputs):
        query_now, current_key, current_value, decay_now = inputs
        running_total = jnp.cumsum(decay_now, axis=1)
        final_entry = running_total[:, -1:, :]
        scaled_query = query_now * jnp.exp(running_total)
        key_scaled = current_key * jnp.exp(-running_total)
        attention_scores = jnp.einsum('hik,hjk->hij', scaled_query, key_scaled, precision=UPPER_PRECISION) * lower
        output_rows = jnp.einsum('daw,dwk->dak', attention_scores, current_value, precision=UPPER_PRECISION) + jnp.einsum('fmb,fbw->fmw', scaled_query, recurrent_state, precision=UPPER_PRECISION)
        state_update = jnp.einsum('adp,adi->api', current_key * jnp.exp(final_entry - running_total), current_value, precision=UPPER_PRECISION)
        recurrent_state = jnp.exp(final_entry[:, 0, :])[:, :, None] * recurrent_state + state_update
        return (recurrent_state, output_rows)
    final_state, attended = lax.scan(step, start_state, (query_blocks, key_blocks, value_blocks, decay_blocks))
    mean_square = lax.optimization_barrier(jnp.mean(attended * attended, axis=3, keepdims=True))
    attn_out = (attended * lax.rsqrt(mean_square + RMS_EPS) * head_gain).astype(jnp.bfloat16)
    attn_out = attn_out.transpose(0, 2, 1, 3).reshape(LENGTH, GVW)
    conv_value = jnp.dot(normed, w_conv_value, preferred_element_type=jnp.float32)
    conv_gate = jnp.dot(normed, w_conv_gate, preferred_element_type=jnp.float32)
    glu = rounded(conv_value * jax.nn.sigmoid(conv_gate))
    padded = jnp.pad(glu, ((KW - 1, 0), (0, 0)))
    filtered = jnp.zeros((LENGTH, CW), jnp.float32)
    for tap_index in range(KW):
        filtered = filtered + conv_taps[tap_index] * padded[tap_index:tap_index + LENGTH]
    mean = lax.optimization_barrier(jnp.mean(filtered, axis=1, keepdims=True))
    centered = filtered - mean
    variance = lax.optimization_barrier(jnp.mean(centered * centered, axis=1, keepdims=True))
    conv_out = jax.nn.silu(centered * lax.rsqrt(variance + LN_EPS) * channel_gain).astype(jnp.bfloat16)
    joined = jnp.concatenate([attn_out, conv_out], axis=1)
    weights = jnp.concatenate([w_out_attn, w_out_conv], axis=0)
    return jnp.dot(joined, weights, preferred_element_type=jnp.float32).astype(jnp.bfloat16)

def reference(tokens, norm_gain, w_query, w_key, w_value, w_conv_value, w_conv_gate, w_decay_low, w_decay_high, gate_bias, decay_shift, head_gain, conv_taps, channel_gain, w_out_attn, w_out_conv, init_state):

    def per_sequence(items):
        return one_sequence(items[0], items[1], items[2], norm_gain, w_query, w_key, w_value, w_conv_value, w_conv_gate, w_decay_low, w_decay_high, gate_bias, head_gain, conv_taps, channel_gain, w_out_attn, w_out_conv)
    return lax.map(per_sequence, (tokens, decay_shift, init_state))
```

```python
import jax
import jax.numpy as jnp
from jax import lax
from jax.experimental import pallas as pl
from jax.experimental.pallas import tpu as pltpu
from jax.sharding import PartitionSpec as P

DK = 256
DV = 512
CW = 1024
KW = 31
BLOCK = 64


RMS_EPS = 1e-06
LN_EPS = 1e-05
GATE_NORMALIZER = 16.0
UPPER_PRECISION = lax.Precision.HIGHEST


def shifted(value, axis, steps):
    count = lax.axis_size(axis)
    initial, last = (max(0, -steps), min(count, count - steps))
    return lax.ppermute(value, axis, [(source, source + steps) for source in range(initial, last)])


def after(value, *earlier):
    return lax.optimization_barrier((value,) + earlier)[0]


def spread_sp(piece, axis):
    count, place = (lax.axis_size("sp"), lax.axis_index("sp"))
    if count > 4:
        return lax.all_gather(piece, "sp", axis=axis, tiled=True)
    size = piece.shape[axis]
    shape = list(piece.shape)
    shape[axis] = size * count
    whole = jnp.zeros(shape, piece.dtype)
    parts = [piece] + [
        lax.ppermute(piece, "sp", [(i, (i + k) % count) for i in range(count)])
        for k in range(1, count)
    ]
    for k, part in enumerate(parts):
        source = (place - k + count) % count
        whole = lax.dynamic_update_slice_in_dim(whole, part, source * size, axis)
    return whole


def spread_fs(part):
    count, place = (lax.axis_size("fs"), lax.axis_index("fs"))
    if count != 4:
        everything = lax.all_gather(part, "fs")
        return [(g, everything[g]) for g in range(count)]

    def swap(value, bit):
        return lax.ppermute(value, "fs", [(i, i ^ bit) for i in range(count)])

    half = part.shape[0] // 2
    one = swap(part, 1)
    two = swap(part, 2)
    upper = swap(two[:half], 1)
    lower = swap(one[half:], 2)
    both = jnp.concatenate([upper, lower], axis=0)
    return [(place, part), (place ^ 1, one), (place ^ 2, two), (place ^ 3, both)]


def split(array):
    high = array.astype(jnp.bfloat16)
    return high, (array - high.astype(jnp.float32)).astype(jnp.bfloat16)


def product(a, b, dims):
    return lax.dot_general(a, b, (dims, ((), ())), preferred_element_type=jnp.float32)


def recurrence(q_ref, k_ref, v_ref, decay_ref, inner_ref, query_ref, end_ref, total_ref, state, start):
    block = pl.program_id(1)

    @pl.when(block == 0)
    def _():
        state[...] = jnp.zeros_like(state)
        start[...] = jnp.zeros_like(start)

    rows = q_ref.shape[0]
    decay = decay_ref[...]
    i = lax.broadcasted_iota(jnp.int32, (rows, rows), 0)
    j = lax.broadcasted_iota(jnp.int32, (rows, rows), 1)
    lower = i >= j
    running = lax.dot_general(
        lower.astype(jnp.float32),
        decay,
        (((1,), (0,)), ((), ())),
        precision=UPPER_PRECISION,
        preferred_element_type=jnp.float32,
    )
    column = lax.dot_general(
        decay,
        jnp.ones((rows, 128), jnp.float32),
        (((0,), (0,)), ((), ())),
        precision=UPPER_PRECISION,
        preferred_element_type=jnp.float32,
    )
    final = running[rows - 1 :, :]
    key = k_ref[...].astype(jnp.float32)
    value = v_ref[...]
    query = q_ref[...].astype(jnp.float32) * DK ** (-0.5) * jnp.exp(running)
    q_hi, q_lo = split(query)
    k_hi, k_lo = split(key * jnp.exp(-running))
    rc = ((1,), (1,))
    scores = product(q_hi, k_hi, rc) + product(q_hi, k_lo, rc) + product(q_lo, k_hi, rc)
    s_hi, s_lo = split(jnp.where(lower, scores, 0.0))
    m_hi, m_lo = split(state[...])
    mm = ((1,), (0,))
    inner_ref[...] = (
        product(s_hi, value, mm)
        + product(s_lo, value, mm)
        + product(q_hi, m_hi, mm)
        + product(q_hi, m_lo, mm)
        + product(q_lo, m_hi, mm)
    )
    d_hi, d_lo = split(key * jnp.exp(final - running))
    tt = ((0,), (0,))
    update = product(d_hi, value, tt) + product(d_lo, value, tt)
    factor = jnp.exp(column)
    state[...] = jnp.concatenate([factor] * (state.shape[1] // 128), axis=1) * state[...] + update
    query_ref[...] = query * jnp.exp(start[...])
    start[...] = start[...] + final

    @pl.when(block == pl.num_programs(1) - 1)
    def _():
        end_ref[...] = state[...]
        total_ref[...] = jnp.exp(start[...])


def local_attention(queries, keys, values, log_decay):
    length = queries.shape[0]
    heads = queries.shape[1] // DK
    key_spec = pl.BlockSpec((BLOCK, DK), lambda h, n: (n, h))
    value_spec = pl.BlockSpec((BLOCK, DV), lambda h, n: (n, h))
    return pl.pallas_call(
        recurrence,
        grid=(heads, length // BLOCK),
        in_specs=[key_spec, key_spec, value_spec, key_spec],
        out_specs=[
            value_spec,
            key_spec,
            pl.BlockSpec((None, DK, DV), lambda h, n: (h, 0, 0)),
            pl.BlockSpec((None, 1, DK), lambda h, n: (h, 0, 0)),
        ],
        out_shape=[
            jax.ShapeDtypeStruct((length, heads * DV), jnp.float32),
            jax.ShapeDtypeStruct((length, heads * DK), jnp.float32),
            jax.ShapeDtypeStruct((heads, DK, DV), jnp.float32),
            jax.ShapeDtypeStruct((heads, 1, DK), jnp.float32),
        ],
        scratch_shapes=[pltpu.VMEM((DK, DV), jnp.float32), pltpu.VMEM((1, DK), jnp.float32)],
        compiler_params=pltpu.CompilerParams(dimension_semantics=("arbitrary", "arbitrary")),
    )(queries, keys, values, log_decay)


def entering(decay, end, initial):
    count, place = (lax.axis_size("sp"), lax.axis_index("sp"))
    if count > 4:
        decays = lax.all_gather(decay, "sp")
        ends = lax.all_gather(end, "sp")

        def turn(k, state):
            return jnp.where(k < place, decays[k][..., None] * state + ends[k], state)

        return lax.fori_loop(0, count, turn, initial)
    incoming = initial
    for k in range(count - 1):
        leaving = (decay[..., None] * incoming + end).astype(jnp.bfloat16)
        arrived = lax.optimization_barrier(lax.ppermute(leaving, "sp", [(k, k + 1)]))
        incoming = jnp.where(place == k + 1, arrived.astype(jnp.float32), incoming)
    return incoming


def on_device(
    tokens,
    norm_gain,
    w_query,
    w_key,
    w_value,
    w_conv_value,
    w_conv_gate,
    w_decay_low,
    w_decay_high,
    gate_bias,
    decay_shift,
    head_gain,
    conv_taps,
    channel_gain,
    w_out_attn,
    w_out_conv,
    init_state,
):
    position = lax.axis_index("tp")
    sp_count = lax.axis_size("sp")
    fs_count = lax.axis_size("fs")
    fs_place = lax.axis_index("fs")
    key_cols = w_query.shape[1]
    value_cols = w_value.shape[1]
    conv_cols = w_conv_value.shape[1]
    heads_here = key_cols // DK

    def quarter(weight):
        rows = weight.shape[0] // fs_count
        return lax.dynamic_slice_in_dim(weight, fs_place * rows, rows, 0)

    first = jnp.concatenate([quarter(w) for w in (w_query, w_key, w_value)], axis=1)
    second = jnp.concatenate([quarter(w) for w in (w_conv_value, w_conv_gate)], axis=1)
    third = jnp.concatenate([quarter(w) for w in (w_out_attn, w_out_conv)], axis=0)
    first = spread_sp(first, 0)
    second = spread_sp(after(second, first), 0)
    first = spread_fs(first)
    third = spread_sp(after(third, second), 1)
    second = spread_fs(after(second, *[w for _, w in first]))
    third = spread_fs(after(third, *[w for _, w in second]))

    token_rows = tokens[0].astype(jnp.float32)
    length_here, width = token_rows.shape
    normed = (
        token_rows
        * lax.rsqrt(jnp.mean(token_rows * token_rows, axis=1, keepdims=True) + RMS_EPS)
        * norm_gain
    ).astype(jnp.bfloat16)
    pieces = normed.reshape(length_here, sp_count, fs_count, -1)

    def features_of(index):
        part = lax.dynamic_slice_in_dim(pieces, index, 1, 2)
        return part.reshape(length_here, width // fs_count)

    features = {g: features_of(index) for g, (index, _) in enumerate(first)}

    def projected(group):
        total = None
        for g, (_, weight) in enumerate(group):
            part = jnp.dot(features[g], weight, preferred_element_type=jnp.float32)
            total = part if total is None else total + part
        return total

    low_rank = jnp.dot(normed, w_decay_low, preferred_element_type=jnp.float32).astype(jnp.bfloat16)
    high_cols = lax.dynamic_slice_in_dim(w_decay_high, position * key_cols, key_cols, 1)
    bias_here = lax.dynamic_slice_in_dim(gate_bias, position * key_cols, key_cols, 0)
    log_decay = (
        jax.nn.log_sigmoid(
            jnp.dot(low_rank, high_cols, preferred_element_type=jnp.float32) + bias_here
        )
        / GATE_NORMALIZER
        + decay_shift[0]
    )
    qkv = projected(first).astype(jnp.bfloat16)
    inner, scaled_query, local_end, device_decay = local_attention(
        qkv[:, :key_cols], qkv[:, key_cols : 2 * key_cols], qkv[:, 2 * key_cols :], log_decay
    )
    incoming_carry = entering(device_decay[:, 0, :], local_end, init_state[0])

    both = projected(second)
    glu = (both[:, :conv_cols] * jax.nn.sigmoid(both[:, conv_cols:])).astype(jnp.bfloat16)
    rim = shifted(glu[length_here - (KW - 1) :], "sp", 1)
    padded = jnp.concatenate([rim, glu], axis=0).astype(jnp.float32)
    taps_here = lax.dynamic_slice_in_dim(conv_taps, position * conv_cols, conv_cols, 1)
    filtered = jnp.zeros((length_here, conv_cols), jnp.float32)
    for tap_index in range(KW):
        filtered = filtered + taps_here[tap_index] * padded[tap_index : tap_index + length_here]
    first_sum, square_sum = lax.psum(
        (
            jnp.sum(filtered, axis=1, keepdims=True),
            jnp.sum(filtered * filtered, axis=1, keepdims=True),
        ),
        "tp",
    )
    channels = conv_taps.shape[1]
    mean = first_sum / channels
    centered = filtered - mean
    variance = square_sum / channels - mean * mean
    gain_here = lax.dynamic_slice_in_dim(channel_gain, position * conv_cols, conv_cols, 0)
    conv_out = jax.nn.silu(centered * lax.rsqrt(variance + LN_EPS) * gain_here).astype(jnp.bfloat16)

    attended = inner.reshape(length_here, heads_here, DV) + jnp.einsum(
        "thk,hkv->thv",
        scaled_query.reshape(length_here, heads_here, DK),
        incoming_carry,
        precision=lax.Precision.HIGH,
    )
    mean_square = jnp.mean(attended * attended, axis=2, keepdims=True)
    attn_out = (attended * lax.rsqrt(mean_square + RMS_EPS) * head_gain).astype(jnp.bfloat16)
    attn_out = attn_out.reshape(length_here, value_cols)

    attn_rows = value_cols // fs_count
    conv_rows = conv_cols // fs_count
    half = length_here // lax.axis_size("tp")

    def columns(start):
        attn_here = lax.dynamic_slice_in_dim(attn_out, start, half, 0)
        conv_here = lax.dynamic_slice_in_dim(conv_out, start, half, 0)
        total = None
        for index, weight in third:
            rows = jnp.concatenate(
                [
                    lax.dynamic_slice_in_dim(attn_here, index * attn_rows, attn_rows, 1),
                    lax.dynamic_slice_in_dim(conv_here, index * conv_rows, conv_rows, 1),
                ],
                axis=1,
            )
            part = jnp.dot(rows, weight, preferred_element_type=jnp.float32)
            total = part if total is None else total + part
        return total

    if lax.axis_size("tp") == 2:
        leaving = columns((1 - position) * half).astype(jnp.bfloat16)
        arrived = lax.ppermute(leaving, "tp", [(0, 1), (1, 0)])
        mixed = columns(position * half) + arrived.astype(jnp.float32)
    else:
        total = jnp.concatenate([columns(k * half) for k in range(lax.axis_size("tp"))], axis=0)
        mixed = lax.psum_scatter(total, "tp", scatter_dimension=0, tiled=True)
    return mixed.astype(jnp.bfloat16)[None]


def solution(mesh):
    in_specs = (
        P("fs", "sp", None),
        P(),
        P("sp", "tp"),
        P("sp", "tp"),
        P("sp", "tp"),
        P("sp", "tp"),
        P("sp", "tp"),
        P(),
        P(),
        P(),
        P("fs", "sp", "tp"),
        P(),
        P(),
        P(),
        P("tp", "sp"),
        P("tp", "sp"),
        P("fs", "tp", None, None),
    )
    out_specs = P("fs", ("sp", "tp"), None)
    return jax.shard_map(
        on_device, mesh=mesh, in_specs=in_specs, out_specs=out_specs, check_vma=False
    )
```
